128 devices in a mesh: grp: 4 (over y, x), tp: 32 (over z, core).
Axes of the slice: x: 2, y: 2, z: 16, core: 2. Of those that a mesh axis runs over, the one named last changes fastest.
The devices are a block of a 8x8x16 slice.
Arguments:
- tokens: bfloat16 [4096, 2048], P('grp', 'tp'), parts along dimension 0, may hold values from -8 to 8
- carried: float32 [2, 2, 32, 64, 4096], P(None, None, 'tp', None, 'grp'), parts along dimension 4, may hold values from -3 to 3
- proj_in: bfloat16 [2, 2048, 512], P(None, None, 'tp'), may hold values from -0.125 to 0.125
- proj_gate: bfloat16 [2, 2048, 512], P(None, None, 'tp'), may hold values from -0.125 to 0.125
- proj_out: bfloat16 [2, 512, 2048], P(None, None, 'tp'), may hold values from -0.5 to 0.5
- norm_params: bfloat16 [2, 2, 2048], P(None, None, 'tp'), may hold values from -0.5 to 2.4
- lambda_re: float32 [2, 32, 64], P(None, 'tp'), may hold values from -1 to -0.05
- lambda_im: float32 [2, 32, 64], P(None, 'tp'), may hold values from -3 to 3
- log_step: float32 [2, 32], P(None, 'tp'), may hold values from -3 to 0
- in_coupling: float32 [2, 2, 32, 64, 16], P(None, None, 'tp'), may hold values from -1 to 1
- out_coupling: float32 [2, 2, 32, 16, 64], P(None, None, 'tp'), may hold values from -1.5 to 1.5
- skip_gain: float32 [2, 512], P(None, 'tp'), may hold values from -4 to 4
Outputs:
- stream_out: bfloat16 [4096, 2048], P('grp', 'tp'), parts along dimension 0
- new_carried: float32 [2, 2, 32, 64, 4096], P(None, None, 'tp', None, 'grp'), parts along dimension 4
The draws below stay inside these ranges and needn't reach their ends.
There are 4 independent parts, one for each index of `grp`. The reference program is written for one: setup_inputs(seed, part) draws one part's arguments, and reference() takes and returns one part's arrays. A program takes and returns all parts, laid end to end along the dimension named above; an argument that names none is the same for every part. Nothing has to cross between parts.
All inputs are finite; a program needn't handle non-finite values.
Results may differ from the reference program's by a relative error of at most 0.015.
Values may be sent and summed in bfloat16 or wider, within the bound.
A program may use at most 64 MiB of HBM per device.

```python
import jax
import jax.numpy as jnp
from jax import lax

D = 2048
GROUPS = 32
GROUP_CH = 16
STATE = 64
SSM = 512
LAYERS = 2
BATCH = 1024


def draw_tokens(key, part):
    keys = jax.random.split(jax.random.fold_in(key, 11), 3)
    base = jax.random.normal(keys[0], (BATCH, D), jnp.float32)
    ramp = jnp.exp(jnp.linspace(jnp.log(0.4), jnp.log(1.6), D)) * jax.random.uniform(keys[1], (D,), jnp.float32, 0.7, 1.3)
    scales = jnp.exp(jax.random.uniform(keys[2], (BATCH, 1), jnp.float32, jnp.log(0.5), jnp.log(2.0)))
    values = base * ramp[None, :] * scales
    return jnp.clip(values, -8.0, 8.0).astype(jnp.bfloat16)


def draw_norm_params(key, part):
    keys = jax.random.split(jax.random.fold_in(key, 23), 2)
    ramp = jnp.exp(jnp.linspace(jnp.log(0.6), jnp.log(1.8), D))
    gains = ramp[None, :] * jax.random.uniform(keys[0], (LAYERS, D), jnp.float32, 0.8, 1.2)
    biases = jax.random.uniform(keys[1], (LAYERS, D), jnp.float32, -0.4, 0.4)
    return jnp.stack([gains, biases], axis=1).astype(jnp.bfloat16)


def steps_of(own_key, extent, pieces, low, top_value):
    factor_of = 1.0
    for dim, shards_of in pieces:
        heights = jax.random.uniform(jax.random.fold_in(jax.random.fold_in(own_key, 6), dim), (shards_of,), jnp.float32, low / len(pieces), top_value / len(pieces))
        factor_of = factor_of * jnp.repeat(jnp.exp(heights), extent[dim] // shards_of).reshape((-1,) + (1,) * (len(extent) - 1 - dim))
    return factor_of


def scatter_about(own_key, shape, spread, reach, cuts=(), held_as=jnp.bfloat16):
    loudness = steps_of(own_key, shape, cuts, -0.22, 0.18) if cuts else 1.0
    array = jax.random.normal(own_key, shape, jnp.float32) * spread * loudness
    return jnp.minimum(jnp.maximum(array, -reach), reach).astype(held_as)


def setup_inputs(seed: int = 0, part: int = 0) -> dict:
    splits = jax.random.split(jax.random.key(seed), 13)
    own_keys = jax.random.split(jax.random.fold_in(splits[12], part), 13)
    tokens = draw_tokens(jax.random.fold_in(jax.random.fold_in(splits[12], part), 71), part)
    carried = scatter_about(own_keys[1], (LAYERS, 2, GROUPS, STATE, BATCH), 0.3, 3.0, ((2, 32),), jnp.float32)
    proj_in = scatter_about(splits[2], (LAYERS, D, SSM), D ** -0.5, 0.125, ((2, 32),))
    proj_gate = scatter_about(splits[3], (LAYERS, D, SSM), D ** -0.5, 0.125, ((2, 32),))
    proj_out = scatter_about(splits[4], (LAYERS, SSM, D), (SSM // 4) ** -0.5, 0.5, ((2, 32),))
    norm_params = draw_norm_params(jax.random.fold_in(splits[12], 71), part)
    lambda_re = jnp.clip(-1.0 + 0.95 * jax.random.uniform(splits[6], (LAYERS, GROUPS, STATE), jnp.float32) ** steps_of(splits[6], (LAYERS, GROUPS, STATE), ((1, 32),), -0.2, 0.2), -1.0, -0.05)
    lambda_im = jnp.clip(jax.random.uniform(splits[7], (LAYERS, GROUPS, STATE), jnp.float32, -3.0, 3.0) * steps_of(splits[7], (LAYERS, GROUPS, STATE), ((1, 32),), -0.4, 0.0), -3.0, 3.0)
    log_step = jnp.clip(-3.0 + 3.0 * jax.random.uniform(splits[8], (LAYERS, GROUPS), jnp.float32) ** steps_of(splits[8], (LAYERS, GROUPS), ((1, 32),), -0.2, 0.2), -3.0, 0.0)
    in_coupling = scatter_about(splits[9], (LAYERS, 2, GROUPS, STATE, GROUP_CH), (2 * GROUP_CH) ** -0.5, 1.0, ((2, 32),), jnp.float32)
    out_coupling = scatter_about(splits[10], (LAYERS, 2, GROUPS, GROUP_CH, STATE), (STATE // 4) ** -0.5, 1.5, ((2, 32),), jnp.float32)
    skip_gain = scatter_about(splits[11], (LAYERS, SSM), 1.0, 4.0, ((1, 32),), jnp.float32)
    return dict(tokens=tokens, carried=carried, proj_in=proj_in, proj_gate=proj_gate, proj_out=proj_out, norm_params=norm_params, lambda_re=lambda_re, lambda_im=lambda_im, log_step=log_step, in_coupling=in_coupling, out_coupling=out_coupling, skip_gain=skip_gain)


residual_scale = 1.4142135623730951
norm_eps = 1e-05
highest_precision = lax.Precision.HIGHEST

def discretize(lam_re, lam_im, log_dt, coupling):
    step_len = jnp.exp(log_dt)[:, None]
    modulus = jnp.exp(lam_re * step_len)
    decay_re = modulus * jnp.cos(lam_im * step_len)
    decay_im = modulus * jnp.sin(lam_im * step_len)
    denominator = lam_re * lam_re + lam_im * lam_im
    shifted = decay_re - 1.0
    coef_re = (shifted * lam_re + decay_im * lam_im) / denominator
    coef_im = (decay_im * lam_re - shifted * lam_im) / denominator
    in_re = coef_re[..., None] * coupling[0] - coef_im[..., None] * coupling[1]
    in_im = coef_re[..., None] * coupling[1] + coef_im[..., None] * coupling[0]
    return (decay_re, decay_im, in_re, in_im)

def recur(drive, gate_pre, states, lam_re, lam_im, log_dt, in_c, output_coupling, skip_connection):
    channel_groups = lam_re.shape[0]
    batch_rows = drive.shape[0]
    drive_expanded = drive.astype(jnp.float32).reshape(batch_rows, channel_groups, -1)
    decay_re, decay_im, in_re, in_im = discretize(lam_re, lam_im, log_dt, in_c)
    push_re = jnp.einsum('bgc,gpc->gpb', drive_expanded, in_re, precision=highest_precision)
    push_im = jnp.einsum('bgc,gpc->gpb', drive_expanded, in_im, precision=highest_precision)
    fresh_real = decay_re[..., None] * states[0] - decay_im[..., None] * states[1] + push_re
    fresh_imaginary = decay_re[..., None] * states[1] + decay_im[..., None] * states[0] + push_im
    readout_rows = jnp.einsum('jyn,jmy->njm', fresh_real, output_coupling[0], precision=highest_precision) - jnp.einsum('jyn,jmy->njm', fresh_imaginary, output_coupling[1], precision=highest_precision) + skip_connection.reshape(channel_groups, -1) * drive_expanded
    readout_rows = readout_rows.reshape(batch_rows, -1)
    gated = (jax.nn.gelu(readout_rows) * jax.nn.sigmoid(gate_pre.astype(jnp.float32))).astype(jnp.bfloat16)
    return (gated, jnp.stack([fresh_real, fresh_imaginary]))

def norm_rows(summed, params):
    wide = summed.astype(jnp.float32)
    mean_row = lax.optimization_barrier(jnp.mean(wide, axis=-1, keepdims=True))
    var_row = lax.optimization_barrier(jnp.mean(wide * wide, axis=-1, keepdims=True)) - mean_row * mean_row
    scaled = (wide - mean_row) * lax.rsqrt(var_row + norm_eps)
    return (scaled * params[0].astype(jnp.float32) + params[1].astype(jnp.float32)).astype(jnp.bfloat16)

def reference(tokens, carried, proj_in, proj_gate, proj_out, norm_params, lambda_re, lambda_im, log_step, in_coupling, out_coupling, skip_gain):
    stream = tokens
    new_states = []
    for layer_idx in range(LAYERS):
        drive = jnp.dot(stream, proj_in[layer_idx], preferred_element_type=jnp.float32).astype(jnp.bfloat16)
        gate_pre = jnp.dot(stream, proj_gate[layer_idx], preferred_element_type=jnp.float32).astype(jnp.bfloat16)
        gated, states = recur(drive, gate_pre, carried[layer_idx], lambda_re[layer_idx], lambda_im[layer_idx], log_step[layer_idx], in_coupling[layer_idx], out_coupling[layer_idx], skip_gain[layer_idx])
        mixed = jnp.dot(gated, proj_out[layer_idx], preferred_element_type=jnp.float32)
        summed = (residual_scale * stream.astype(jnp.float32) + mixed).astype(jnp.bfloat16)
        stream = norm_rows(summed, norm_params[layer_idx])
        new_states.append(states)
    return (stream, jnp.stack(new_states))
```

```python
import functools

import jax
import jax.numpy as jnp
from jax import lax
from jax.experimental import pallas as pl
from jax.experimental.pallas import tpu as pltpu
from jax.sharding import PartitionSpec as P

MESH = pl.DeviceIdType.MESH
bf16, f32 = jnp.bfloat16, jnp.float32

residual_scale = 1.4142135623730951
norm_eps = 1e-05


def tile(start, size):
    return pl.ds(pl.multiple_of(start, size), size)


class Ring:
    def __init__(self, nz, own, buf, per, pieces, send, recv, give, take):
        self.nz, self.own, self.buf, self.per, self.pieces = nz, own, buf, per, pieces
        self.send_sem, self.recv_sem, self.give_sem, self.take_sem = send, recv, give, take
        me = lax.axis_index("tp")
        self.z, self.c = me // 2, lax.rem(me, 2)
        self.me, self.sib = me, self.z * 2 + (1 - self.c)
        self.next = (lax.rem(self.z + 1, nz) * 2 + self.c, lax.rem(self.z + nz - 1, nz) * 2 + self.c)
        self.half = nz // 2

    def origin(self, way, s, core):
        z = lax.rem(self.z - s + self.nz, self.nz) if way == 0 else lax.rem(self.z + s, self.nz)
        return z * 2 + core

    def parts(self, way, s):
        if s < self.half:
            n = self.pieces
            return [(i * self.per // n, self.per // n) for i in range(n)]
        return [(way * self.per // 2, self.per // 2)]

    def place(self, dev, part):
        start, size = part
        return self.buf.at[pl.ds(pl.multiple_of(dev * self.per + start, size), size)]

    def hop(self, way, s, i):
        part = self.parts(way, s)[i]
        src_dev = self.origin(way, s - 1, self.c)
        src = self.own.at[pl.ds(*part)] if s == 1 and self.own is not None else self.place(src_dev, part)
        return pltpu.make_async_remote_copy(
            src_ref=src,
            dst_ref=self.place(src_dev, part),
            send_sem=self.send_sem.at[way, s - 1, i],
            recv_sem=self.recv_sem.at[way, s - 1, i],
            device_id={"tp": self.next[way]},
            device_id_type=MESH,
        )

    def start(self, way, s, i):
        self.hop(way, s, i).start()

    def arrive(self, way, s, i):
        part = self.parts(way, s)[i]
        dst = self.place(self.origin(way, s, self.c), part)
        pltpu.make_async_remote_copy(
            src_ref=dst,
            dst_ref=dst,
            send_sem=self.send_sem.at[way, s - 1, i],
            recv_sem=self.recv_sem.at[way, s - 1, i],
            device_id={"tp": self.next[way]},
            device_id_type=MESH,
        ).wait_recv()

    def whole(self, way, s):
        return (0, self.per) if s < self.half else self.parts(way, s)[0]

    def handover(self, way, s, core):
        part = self.whole(way, s)
        dev = self.origin(way, s, core)
        src = self.own if s == 0 and self.own is not None else self.place(dev, part)
        return pltpu.make_async_remote_copy(
            src_ref=src,
            dst_ref=self.place(dev, part),
            send_sem=self.give_sem.at[way, s],
            recv_sem=self.take_sem.at[way, s],
            device_id={"tp": self.sib},
            device_id_type=MESH,
        )

    def begin(self):
        for i in range(self.pieces):
            for way in range(2):
                if self.half > 1:
                    self.start(way, 1, i)
        if self.half == 1:
            for way in range(2):
                self.start(way, 1, 0)
        self.handover(0, 0, self.c).start()

    def step(self, s):
        n = max(len(self.parts(0, s)), 1)
        for i in range(n):
            for way in range(2):
                self.arrive(way, s, i)
                if s + 1 < self.half:
                    self.start(way, s + 1, i)
        if s + 1 == self.half:
            for way in range(2):
                self.start(way, s + 1, 0)
        for way in range(2):
            self.handover(way, s, self.c).start()

    def other(self, s):
        for way in range(2 if s else 1):
            dev = self.origin(way, s, 1 - self.c)
            dst = self.place(dev, self.whole(way, s))
            pltpu.make_async_remote_copy(
                src_ref=dst,
                dst_ref=dst,
                send_sem=self.give_sem.at[way, s],
                recv_sem=self.take_sem.at[way, s],
                device_id={"tp": self.sib},
                device_id_type=MESH,
            ).wait_recv()

    def finish(self):
        for s in range(1, self.half + 1):
            for way in range(2):
                for i in range(len(self.parts(way, s))):
                    self.hop(way, s, i).wait_send()
        for s in range(self.half + 1):
            for way in range(2 if s else 1):
                self.handover(way, s, self.c).wait_send()


def dot(a, b):
    return jnp.dot(a, b, preferred_element_type=f32)


def kernel(
    nz,
    tok,
    carried,
    win,
    wgate,
    wout,
    norm,
    lam_re,
    lam_im,
    log_step,
    in_c,
    out_c,
    skip,
    out,
    new_carried,
    x_all,
    s_all,
    w_all,
    g_all,
    p_own,
    p_all,
    gain_b,
    bias_b,
    w_in,
    push_w,
    push_t,
    read_w,
    cols,
    cols_t,
    held,
    fresh,
    acc,
    x_sem,
    xd_sem,
    w_sem,
    wd_sem,
    g_sem,
    gd_sem,
    p_sem,
    pd_sem,
    io_sem,
):
    layers, half = 2, nz // 2
    ndev = 2 * nz
    width, batch = x_all.shape
    per = tok.shape[0]
    ch = win.shape[1]
    state = held.shape[2]
    me = lax.axis_index("tp")

    xr = Ring(nz, tok, x_all, per, 2, x_sem.at[0], x_sem.at[1], xd_sem.at[0], xd_sem.at[1])
    pr = Ring(nz, p_own, p_all, 16, 1, p_sem.at[0], p_sem.at[1], pd_sem.at[0], pd_sem.at[1])
    wr = [
        Ring(nz, wout.at[i], w_all.at[i], per, 1, w_sem.at[i, 0], w_sem.at[i, 1], wd_sem.at[i, 0], wd_sem.at[i, 1])
        for i in range(layers)
    ]
    gr = [
        Ring(nz, None, g_all.at[i], ch, 1, g_sem.at[i, 0], g_sem.at[i, 1], gd_sem.at[i, 0], gd_sem.at[i, 1])
        for i in range(layers)
    ]

    barrier = pltpu.get_barrier_semaphore()
    for dev in (*xr.next, xr.sib):
        pl.semaphore_signal(barrier, inc=1, device_id={"tp": dev}, device_id_type=MESH)
    load = pltpu.make_async_copy(carried, held, io_sem.at[0])
    load.start()
    p_own[...] = jnp.zeros_like(p_own)
    p_own[0:4, 0:per] = norm[...].astype(f32)
    pl.semaphore_wait(barrier, 3)

    xr.begin()
    pr.begin()

    x_all[tile(me * per, per)] = tok[...]
    p_all[tile(me * 16, 16)] = p_own[...]
    for l in range(layers):
        w_all[l, tile(me * per, per)] = wout[l]
        w_in[l, 0:ch] = win[l]
        w_in[l, ch : 2 * ch] = wgate[l]
    cols[...] = jnp.zeros_like(cols)
    for l in range(layers):
        re, im = lam_re[l], lam_im[l]
        step_len = jnp.exp(log_step[l : l + 1, 0:1])
        modulus = jnp.exp(re * step_len)
        decay_re = modulus * jnp.cos(im * step_len)
        decay_im = modulus * jnp.sin(im * step_len)
        denominator = re * re + im * im
        shifted = decay_re - 1.0
        coef_re = (shifted * re + decay_im * im) / denominator
        coef_im = (decay_im * re - shifted * im) / denominator
        in_re = coef_re * in_c[l, 0] - coef_im * in_c[l, 1]
        in_im = coef_re * in_c[l, 1] + coef_im * in_c[l, 0]
        push_t[l] = jnp.zeros_like(push_t[l])
        for k, v in enumerate((in_re, in_im)):
            high = v.astype(bf16).astype(f32)
            push_t[l, 0:ch, k * state : (k + 1) * state] = high
            push_t[l, ch : 2 * ch, k * state : (k + 1) * state] = v - high
        push_w[l] = push_t[l].T.astype(bf16)
        read_w[l, :, 0:state] = out_c[l, 0].astype(bf16)
        read_w[l, :, state : 2 * state] = (-out_c[l, 1]).astype(bf16)
        cols[8 * l : 8 * l + 1, 0:state] = decay_re
        cols[8 * l + 1 : 8 * l + 2, 0:state] = decay_im
        cols[8 * l + 2 : 8 * l + 3, 0:ch] = skip[l : l + 1]
    cols[3:5, 0:per] = norm[2:4].astype(f32)
    cols_t[...] = cols[...].T

    def gain_columns():
        for d in range(ndev):
            if d % 8 == 0:
                turned = p_all[d * 16 : (d + 8) * 16].T
            at = (d % 8) * 16
            gain_b[d * per : (d + 1) * per] = jnp.broadcast_to(turned[0:per, at : at + 1], (per, 128))
            bias_b[d * per : (d + 1) * per] = jnp.broadcast_to(turned[0:per, at + 1 : at + 2], (per, 128))

    def meet(dev_z):
        k = tile(dev_z * 2 * per, 2 * per)
        acc[...] += dot(w_in[0, :, k], x_all[k])

    acc[...] = jnp.zeros_like(acc)
    for s in range(1, half + 1):
        pr.step(s)
        xr.step(s)
        xr.other(s - 1)
        pr.other(s - 1)
        if s == 1:
            meet(xr.z)
        else:
            for way in range(2):
                meet(xr.origin(way, s - 1, 0) // 2)
    wr[0].begin()
    xr.other(half)
    pr.other(half)
    meet(xr.origin(0, half, 0) // 2)

    load.wait()

    def recur(l):
        span = min(256, batch)
        for j in range(batch // span):
            at = slice(j * span, (j + 1) * span)
            drive = acc[0:ch, at].astype(bf16)
            gate = acc[ch : 2 * ch, at].astype(bf16).astype(f32)
            pushed = dot(push_w[l, :, 0 : 2 * ch], jnp.concatenate([drive, drive], axis=0))
            decay_re = cols_t[0:state, 8 * l : 8 * l + 1]
            decay_im = cols_t[0:state, 8 * l + 1 : 8 * l + 2]
            old_re, old_im = held[l, 0, :, at], held[l, 1, :, at]
            re = decay_re * old_re - decay_im * old_im + pushed[0:state]
            im = decay_re * old_im + decay_im * old_re + pushed[state:]
            fresh[l, 0, :, at] = re
            fresh[l, 1, :, at] = im
            both = jnp.concatenate([re.astype(bf16), im.astype(bf16)], axis=0)
            y = dot(read_w[l], both) + cols_t[0:ch, 8 * l + 2 : 8 * l + 3] * drive.astype(f32)
            gated = jax.nn.gelu(y) * jax.nn.sigmoid(gate)
            g_all[l, tile(me * ch, ch), at] = gated.astype(bf16)
        return pltpu.make_async_copy(fresh.at[l], new_carried.at[l], io_sem.at[1 + l])

    def exchange(l):
        gr[l].begin()
        for s in range(1, half + 1):
            gr[l].step(s)
            wr[l].step(s)
            gr[l].other(s - 1)
            wr[l].other(s - 1)
        gr[l].other(half)
        wr[l].other(half)

    rows = 256
    spans = batch // 128

    def moments(l, src, keep):
        def body(t, sums):
            k = tile(t * rows, rows)
            mixed = dot(w_all[l, k], g_all[l])
            summed = (residual_scale * src[k].astype(f32) + mixed).astype(bf16)
            if keep is not None:
                keep[k] = summed
            wide = summed.astype(f32).reshape(rows // 8, 8, batch)
            return sums[0] + wide.sum(axis=0), sums[1] + (wide * wide).sum(axis=0)

        zero = jnp.zeros((8, batch), f32)
        total, squares = lax.fori_loop(0, width // rows, body, (zero, zero))
        mean = total.sum(axis=0, keepdims=True) / width
        var = squares.sum(axis=0, keepdims=True) / width - mean * mean
        return mean, lax.rsqrt(var + norm_eps)

    store = recur(0)
    store.start()
    exchange(0)
    gain_columns()
    mean, scale = moments(0, x_all, s_all)
    acc[...] = jnp.zeros_like(acc)

    def normed(t, _):
        k = tile(t * rows, rows)
        for j in range(spans):
            at = slice(j * 128, (j + 1) * 128)
            wide = (s_all[k, at].astype(f32) - mean[:, at]) * scale[:, at]
            s_all[k, at] = (wide * gain_b[k] + bias_b[k]).astype(bf16)
        acc[...] += dot(w_in[1, :, k], s_all[k])
        return 0

    lax.fori_loop(0, width // rows, normed, 0)
    wr[1].begin()
    store2 = recur(1)
    store2.start()
    exchange(1)
    mean, scale = moments(1, s_all, None)
    mine = tile(me * per, per)
    summed = (residual_scale * s_all[mine].astype(f32) + dot(wout[1], g_all[1])).astype(bf16).astype(f32)
    out[...] = ((summed - mean) * scale * cols_t[0:per, 3:4] + cols_t[0:per, 4:5]).astype(bf16)
    store.wait()
    store2.wait()
    for ring in (xr, pr, *wr, *gr):
        ring.finish()


def per_device(nz, tokens, carried, proj_in, proj_gate, proj_out, norm, lam_re, lam_im, log_step, in_c, out_c, skip):
    batch, per = tokens.shape
    layers, width, ch = proj_in.shape
    ssm = proj_out.shape[1]
    state = carried.shape[3]
    half = nz // 2
    vmem = pl.BlockSpec(memory_space=pltpu.VMEM)
    hbm = pl.BlockSpec(memory_space=pl.ANY)
    dma = pltpu.SemaphoreType.DMA
    out, fresh = pl.pallas_call(
        functools.partial(kernel, nz),
        out_shape=(
            jax.ShapeDtypeStruct((per, batch), bf16),
            jax.ShapeDtypeStruct((layers, 2, state, batch), f32),
        ),
        in_specs=[vmem, hbm] + [vmem] * 10,
        out_specs=(vmem, hbm),
        scratch_shapes=[
            pltpu.VMEM((width, batch), bf16),
            pltpu.VMEM((width, batch), bf16),
            pltpu.VMEM((layers, width, ssm), bf16),
            pltpu.VMEM((layers, ssm, batch), bf16),
            pltpu.VMEM((16, 128), f32),
            pltpu.VMEM((2 * nz * 16, 128), f32),
            pltpu.VMEM((width, 128), f32),
            pltpu.VMEM((width, 128), f32),
            pltpu.VMEM((layers, 2 * ch, width), bf16),
            pltpu.VMEM((layers, 128, 128), bf16),
            pltpu.VMEM((layers, 128, 128), f32),
            pltpu.VMEM((layers, ch, 2 * state), bf16),
            pltpu.VMEM((128, 128), f32),
            pltpu.VMEM((128, 128), f32),
            pltpu.VMEM((layers, 2, state, batch), f32),
            pltpu.VMEM((layers, 2, state, batch), f32),
            pltpu.VMEM((2 * ch, batch), f32),
            dma((2, 2, half, 2)),
            dma((2, 2, half + 1)),
            dma((layers, 2, 2, half, 1)),
            dma((layers, 2, 2, half + 1)),
            dma((layers, 2, 2, half, 1)),
            dma((layers, 2, 2, half + 1)),
            dma((2, 2, half, 1)),
            dma((2, 2, half + 1)),
            dma((3,)),
        ],
        compiler_params=pltpu.CompilerParams(
            collective_id=0, has_side_effects=True, vmem_limit_bytes=56 * 1024 * 1024
        ),
    )(
        tokens.T,
        carried.reshape(layers, 2, state, batch),
        proj_in.transpose(0, 2, 1),
        proj_gate.transpose(0, 2, 1),
        proj_out.transpose(0, 2, 1),
        norm.reshape(2 * layers, per),
        lam_re,
        lam_im,
        log_step,
        in_c.reshape(layers, 2, state, ch).transpose(0, 1, 3, 2),
        out_c.reshape(layers, 2, ch, state),
        skip,
    )
    return out.T, fresh.reshape(carried.shape)


def solution(mesh):
    return jax.shard_map(
        functools.partial(per_device, mesh.shape["tp"] // 2),
        mesh=mesh,
        in_specs=(
            P("grp", "tp"),
            P(None, None, "tp", None, "grp"),
            P(None, None, "tp"),
            P(None, None, "tp"),
            P(None, None, "tp"),
            P(None, None, "tp"),
            P(None, "tp", None),
            P(None, "tp", None),
            P(None, "tp"),
            P(None, None, "tp", None, None),
            P(None, None, "tp", None, None),
            P(None, "tp"),
        ),
        out_specs=(P("grp", "tp"), P(None, None, "tp", None, "grp")),
        check_vma=False,
    )
```

```python
import functools

import jax
import jax.numpy as jnp
from jax import lax
from jax.experimental import pallas as pl
from jax.experimental.pallas import tpu as pltpu
from jax.sharding import PartitionSpec as P

MESH = pl.DeviceIdType.MESH
bf16, f32 = jnp.bfloat16, jnp.float32

residual_scale = 1.4142135623730951
norm_eps = 1e-05

X_PIECES = 2
W_PIECES = 2
STRIDE = 2
W_LEAD = 6
VMEM_MIB = 56
W_RELAY = (1, 0)
P_RELAY = 1


def tile(start, size):
    return pl.ds(pl.multiple_of(start, size), size)


class Place:
    def __init__(self, nz):
        me = lax.axis_index("tp")
        self.nz, self.half = nz, nz // 2
        self.me, self.z, self.c = me, me // 2, lax.rem(me, 2)
        self.sib = self.z * 2 + (1 - self.c)

    def away(self, way, s):
        return lax.rem(self.z + (s if way == 0 else self.nz - s), self.nz)

    def origin(self, way, s):
        return self.away(1 - way, s)

    def carries(self, way, s, core):
        return s < self.half or (s == self.half and (way == 0) == (core == 1))


class Gather:
    def __init__(self, at, relay, own, buf, per, pieces, stride, send, recv, give, take):
        self.relay, self.relays = relay, at.c == relay
        self.at, self.own, self.buf, self.per, self.pieces, self.stride = at, own, buf, per, pieces, stride
        self.send_sem, self.recv_sem, self.give_sem, self.take_sem = send, recv, give, take

    def rows(self, start, size):
        return self.buf.at[pl.ds(pl.multiple_of(start, size), size)]

    def copy(self, way, s, core, i, by=1):
        at, size = self.at, self.per // self.pieces
        chip = at.origin(way, s - by)
        dst = self.rows((chip * 2 + core) * self.per + i * size, size)
        src = dst if s > by or self.own is None else self.own.at[pl.ds(i * size, size)]
        return pltpu.make_async_remote_copy(
            src_ref=src,
            dst_ref=dst,
            send_sem=self.send_sem,
            recv_sem=self.recv_sem.at[way, s - 1, core, i],
            device_id={"tp": at.away(way, by) * 2 + self.relay},
            device_id_type=MESH,
        )

    def arrive(self, way, s, core, i):
        size = self.per // self.pieces
        dst = self.rows((self.at.origin(way, s) * 2 + core) * self.per + i * size, size)
        pltpu.make_async_remote_copy(
            src_ref=dst,
            dst_ref=dst,
            send_sem=self.send_sem,
            recv_sem=self.recv_sem.at[way, s - 1, core, i],
            device_id={"tp": self.at.sib},
            device_id_type=MESH,
        ).wait_recv()

    def reach(self, s):
        if s % self.stride:
            return []
        return [s + by for by in range(self.stride, 0, -1) if s + by <= self.at.half]

    def span(self, way, s):
        chip = self.at.origin(way, s) * 2 * self.per
        if s < self.at.half:
            return self.rows(chip, 2 * self.per)
        return self.rows(chip + (self.per if way == 0 else 0), self.per)

    def handover(self, way, s):
        dst = self.span(way, s)
        return pltpu.make_async_remote_copy(
            src_ref=dst,
            dst_ref=dst,
            send_sem=self.give_sem,
            recv_sem=self.take_sem.at[s],
            device_id={"tp": self.at.sib},
            device_id_type=MESH,
        )

    def own_over(self):
        dst = self.rows(self.at.me * self.per, self.per)
        return pltpu.make_async_remote_copy(
            src_ref=dst if self.own is None else self.own,
            dst_ref=dst,
            send_sem=self.give_sem,
            recv_sem=self.take_sem.at[0],
            device_id={"tp": self.at.sib},
            device_id_type=MESH,
        )

    def sends(self, s, way, core):
        return [t for t in self.reach(s) if self.at.carries(way, t, core)]

    def begin(self):
        for core in range(2):

            @pl.when(self.at.c == core)
            def _():
                for t in self.reach(0):
                    for i in range(self.pieces):
                        for way in range(2):
                            if self.at.carries(way, t, core):
                                self.copy(way, t, core, i, t).start()

        self.own_over().start()

    def order(self):
        half, stride = self.at.half, self.stride
        out = []
        for k in range(0, half, stride):
            top = min(k + stride, half)
            out.append([top] + list(range(k + 1, top)))
        return out

    def step(self, s):
        @pl.when(self.relays)
        def _():
            for core in (self.relay, 1 - self.relay):
                for i in range(self.pieces):
                    for way in range(2):
                        if self.at.carries(way, s, core):
                            self.arrive(way, s, core, i)
                            for t in self.sends(s, way, core):
                                self.copy(way, t, core, i, t - s).start()
            for way in range(2):
                self.handover(way, s).start()

    def bulk(self, blocks, send=None, recv=None):
        ref = self.buf.at[pl.ds(0, blocks * self.per)]
        return pltpu.make_async_remote_copy(
            src_ref=ref,
            dst_ref=ref,
            send_sem=self.send_sem if send is None else send,
            recv_sem=self.take_sem.at[0] if recv is None else recv,
            device_id={"tp": self.at.sib},
            device_id_type=MESH,
        )

    def ready(self, s):
        if s == 0:
            self.bulk(1, recv=self.take_sem.at[0]).wait_recv()
            return

        @pl.when(jnp.logical_not(self.relays))
        def _():
            self.bulk(4 if s < self.at.half else 2, recv=self.take_sem.at[s]).wait_recv()

    def finish(self):
        half, every = self.at.half, [(way, core) for way in range(2) for core in range(2)]
        for core in range(2):
            sent = sum(self.at.carries(way, t, core) for t in self.reach(0) for way in range(2))
            given = 1
            if core == self.relay:
                sent += sum(len(self.sends(s, *who)) for s in range(1, half + 1) for who in every)
                given += 4 * (half - 1) + 2

            @pl.when(self.at.c == core)
            def _():
                self.bulk(sent).wait_send()
                self.bulk(given, send=self.give_sem).wait_send()


def dot(a, b):
    return jnp.dot(a, b, preferred_element_type=f32)


def kernel(
    nz,
    tok_in,
    carried,
    win,
    wgate,
    wout_in,
    norm_in,
    lam_re_in,
    lam_im_in,
    log_step_in,
    in_c_in,
    out_c_in,
    skip_in,
    out_to,
    new_carried,
    tok,
    wout,
    norm,
    lam_re,
    lam_im,
    log_step,
    in_c,
    out_c,
    skip,
    out,
    x_all,
    s_all,
    w_all,
    g_all,
    p_own,
    p_all,
    gain_b,
    bias_b,
    w_in,
    push_w,
    push_t,
    read_w,
    cols,
    cols_t,
    held,
    fresh,
    acc,
    x_sem,
    xd_sem,
    w_sem,
    wd_sem,
    g_sem,
    gd_sem,
    p_sem,
    pd_sem,
    in_sem,
    io_sem,
    sent,
):
    layers, half = 2, nz // 2
    ndev = 2 * nz
    width, batch = x_all.shape
    per = tok.shape[0]
    ch = win.shape[1]
    state = held.shape[2]
    place = Place(nz)
    me = place.me

    def gather(relay, own, buf, rows, pieces, stride, sem, over, out):
        return Gather(place, relay, own, buf, rows, pieces, stride, sent.at[2 * out], sem, sent.at[2 * out + 1], over)

    xr = gather(1, tok, x_all, per, X_PIECES, 1, x_sem, xd_sem, 0)
    pr = gather(P_RELAY, p_own, p_all, 8, 1, 1, p_sem, pd_sem, 1)
    wr = [gather(W_RELAY[i], wout.at[i], w_all.at[i], per, W_PIECES, 1, w_sem.at[i], wd_sem.at[i], 2 + i) for i in range(layers)]
    gr = [gather(1, None, g_all.at[i], ch, 1, STRIDE, g_sem.at[i], gd_sem.at[i], 4 + i) for i in range(layers)]

    barrier = pltpu.get_barrier_semaphore()
    reach = {core: max((r.stride for r in (xr, pr, *wr, *gr) if r.relay == core), default=0) for core in range(2)}

    def near(core):
        return [(way, s) for way in range(2) for s in range(1, min(reach[core], half) + 1) if way == 0 or 2 * s < nz]

    def here(dev):
        pl.semaphore_signal(barrier, inc=1, device_id={"tp": dev}, device_id_type=MESH)

    for core in range(2):

        @pl.when(place.c == core)
        def _():
            for way, s in near(core):
                for other in range(2):
                    here(place.away(way, s) * 2 + other)

    here(place.sib)
    sources = (tok_in, norm_in, wout_in, lam_re_in, lam_im_in, log_step_in, in_c_in, out_c_in, skip_in, carried)
    targets = (tok, norm, wout, lam_re, lam_im, log_step, in_c, out_c, skip, held)
    loads = [pltpu.make_async_copy(a, b, in_sem.at[i]) for i, (a, b) in enumerate(zip(sources, targets))]
    for k, w in enumerate((win, wgate)):
        for l in range(layers):
            part = w_in.at[l, pl.ds(k * ch, ch)]
            loads.append(pltpu.make_async_copy(w.at[l], part, in_sem.at[len(sources) + 2 * k + l]))
    for load in loads:
        load.start()
    loads[0].wait()
    loads[1].wait()
    p_own[...] = jnp.zeros_like(p_own)
    p_own[0:4, 0:per] = norm[...].astype(f32)
    pl.semaphore_wait(barrier, len(near(0)) + len(near(1)) + 1)

    xr.begin()
    pr.begin()
    for i, load in enumerate(loads):
        if i > 1 and i != len(sources) - 1:
            load.wait()

    x_all[tile(me * per, per)] = tok[...]
    p_all[tile(me * 8, 8)] = p_own[...]
    for l in range(layers):
        w_all[l, tile(me * per, per)] = wout[l]
    cols[...] = jnp.zeros_like(cols)
    for l in range(layers):
        re, im = lam_re[l], lam_im[l]
        step_len = jnp.exp(log_step[0:1, l : l + 1])
        modulus = jnp.exp(re * step_len)
        decay_re = modulus * jnp.cos(im * step_len)
        decay_im = modulus * jnp.sin(im * step_len)
        denominator = re * re + im * im
        shifted = decay_re - 1.0
        coef_re = (shifted * re + decay_im * im) / denominator
        coef_im = (decay_im * re - shifted * im) / denominator
        in_re = coef_re * in_c[l, 0] - coef_im * in_c[l, 1]
        in_im = coef_re * in_c[l, 1] + coef_im * in_c[l, 0]
        push_t[l] = jnp.zeros_like(push_t[l])
        for k, v in enumerate((in_re, in_im)):
            high = v.astype(bf16).astype(f32)
            push_t[l, 0:ch, k * state : (k + 1) * state] = high
            push_t[l, ch : 2 * ch, k * state : (k + 1) * state] = v - high
        push_w[l] = push_t[l].T.astype(bf16)
        read_w[l, :, 0:state] = out_c[l, 0].astype(bf16)
        read_w[l, :, state : 2 * state] = (-out_c[l, 1]).astype(bf16)
        cols[8 * l : 8 * l + 1, 0:state] = decay_re
        cols[8 * l + 1 : 8 * l + 2, 0:state] = decay_im
        cols[8 * l + 2 : 8 * l + 3, 0:ch] = skip[l : l + 1]
    cols[3:5, 0:per] = norm[2:4].astype(f32)
    cols_t[...] = cols[...].T

    def gain_columns():
        for d in range(ndev):
            if d % 16 == 0:
                turned = p_all[d * 8 : d * 8 + min(128, ndev * 8)].T
            at = (d % 16) * 8
            gain_b[d * per : (d + 1) * per] = jnp.broadcast_to(turned[0:per, at : at + 1], (per, 128))
            bias_b[d * per : (d + 1) * per] = jnp.broadcast_to(turned[0:per, at + 1 : at + 2], (per, 128))

    def meet(dev_z):
        k = tile(dev_z * 2 * per, 2 * per)
        acc[...] += dot(w_in[0, :, k], x_all[k])

    acc[...] = jnp.zeros_like(acc)
    w_first = max(half + 1 - W_LEAD, 0)
    if w_first == 0:
        wr[0].begin()
    for s in range(1, half + 1):
        xr.step(s)
        if s == w_first:
            wr[0].begin()
        if s > w_first:
            wr[0].step(s - w_first)
        pr.step(s)
        xr.ready(s - 1)
        if s == 1:
            meet(place.z)
        else:
            for way in range(2):
                meet(place.origin(way, s - 1))
    if W_LEAD == 0:
        wr[0].begin()
    xr.ready(half)
    meet(place.origin(0, half))
    w_next = max(min(W_LEAD, half), 1) if w_first else half + 1

    loads[len(sources) - 1].wait()

    def recur(l):
        span = min(256, batch)
        for j in range(batch // span):
            at = slice(j * span, (j + 1) * span)
            drive = acc[0:ch, at].astype(bf16)
            gate = acc[ch : 2 * ch, at].astype(bf16).astype(f32)
            pushed = dot(push_w[l, :, 0 : 2 * ch], jnp.concatenate([drive, drive], axis=0))
            decay_re = cols_t[0:state, 8 * l : 8 * l + 1]
            decay_im = cols_t[0:state, 8 * l + 1 : 8 * l + 2]
            old_re, old_im = held[l, 0, :, at], held[l, 1, :, at]
            re = decay_re * old_re - decay_im * old_im + pushed[0:state]
            im = decay_re * old_im + decay_im * old_re + pushed[state:]
            fresh[l, 0, :, at] = re
            fresh[l, 1, :, at] = im
            both = jnp.concatenate([re.astype(bf16), im.astype(bf16)], axis=0)
            y = dot(read_w[l], both) + cols_t[0:ch, 8 * l + 2 : 8 * l + 3] * drive.astype(f32)
            gated = jax.nn.gelu(y) * jax.nn.sigmoid(gate)
            g_all[l, tile(me * ch, ch), at] = gated.astype(bf16)
        return pltpu.make_async_copy(fresh.at[l], new_carried.at[l], io_sem.at[l])

    w_two = iter(range(half + 1))

    def further():
        s = next(w_two, None)
        if s == 0:
            wr[1].begin()
        elif s is not None:
            wr[1].step(s)

    def exchange(l, left):
        gr[l].begin()
        order = gr[l].order()
        if l == 0:
            further()
            for s in range(half + 1):
                pr.ready(s)
            gain_columns()
        for n, steps in enumerate(order):
            for s in steps:
                gr[l].step(s)
            upto = -(-len(left) // (len(order) - n))
            for s in left[:upto]:
                wr[l].step(s)
            left = left[upto:]
            if l == 0:
                further()
        for s in range(half + 1):
            gr[l].ready(s)
            wr[l].ready(s)

    rows = 256
    spans = batch // 128

    def moments(l, src, keep):
        def body(t, sums):
            k = tile(t * rows, rows)
            mixed = dot(w_all[l, k], g_all[l])
            summed = (residual_scale * src[k].astype(f32) + mixed).astype(bf16)
            if keep is not None:
                keep[k] = summed
            wide = summed.astype(f32).reshape(rows // 8, 8, batch)
            return sums[0] + wide.sum(axis=0), sums[1] + (wide * wide).sum(axis=0)

        zero = jnp.zeros((8, batch), f32)
        sums, tiles = (zero, zero), width // rows
        total, squares = lax.fori_loop(0, tiles, body, sums)
        mean = total.sum(axis=0, keepdims=True) / width
        var = squares.sum(axis=0, keepdims=True) / width - mean * mean
        return mean, lax.rsqrt(var + norm_eps)

    store = recur(0)
    store.start()
    exchange(0, list(range(w_next, half + 1)))
    mean, scale = moments(0, x_all, s_all)
    acc[...] = jnp.zeros_like(acc)

    def normed(t, _):
        k = tile(t * rows, rows)
        for j in range(spans):
            at = slice(j * 128, (j + 1) * 128)
            wide = (s_all[k, at].astype(f32) - mean[:, at]) * scale[:, at]
            s_all[k, at] = (wide * gain_b[k] + bias_b[k]).astype(bf16)
        acc[...] += dot(w_in[1, :, k], s_all[k])
        return 0

    tiles = width // rows
    lax.fori_loop(0, tiles, normed, 0)
    further()
    store2 = recur(1)
    store2.start()
    exchange(1, list(w_two))
    mean, scale = moments(1, s_all, None)
    mine = tile(me * per, per)
    summed = (residual_scale * s_all[mine].astype(f32) + dot(wout[1], g_all[1])).astype(bf16).astype(f32)
    out[...] = ((summed - mean) * scale * cols_t[0:per, 3:4] + cols_t[0:per, 4:5]).astype(bf16)
    last = pltpu.make_async_copy(out, out_to, io_sem.at[2])
    last.start()
    store.wait()
    store2.wait()
    last.wait()
    for ring in (xr, pr, *wr, *gr):
        ring.finish()


def hand_out(out_in, fresh_in, out, fresh, out_held, fresh_held, sem):
    layers = fresh.shape[0]
    pairs = [(out_in, out_held, out)]
    pairs += [(fresh_in.at[l, k], fresh_held.at[l, k], fresh.at[l, k]) for l in range(layers) for k in range(2)]
    into = [pltpu.make_async_copy(a, b, sem.at[0, i]) for i, (a, b, _) in enumerate(pairs)]
    onto = [pltpu.make_async_copy(b, c, sem.at[1, i]) for i, (_, b, c) in enumerate(pairs)]
    for copy in into:
        copy.start()
    for first, then in zip(into, onto):
        first.wait()
        then.start()
    for copy in onto:
        copy.wait()


def per_device(nz, tokens, carried, proj_in, proj_gate, proj_out, norm, lam_re, lam_im, log_step, in_c, out_c, skip):
    batch, per = tokens.shape
    layers, width, ch = proj_in.shape
    ssm = proj_out.shape[1]
    state = carried.shape[3]
    half = nz // 2
    hbm = pl.BlockSpec(memory_space=pl.ANY)
    dma = pltpu.SemaphoreType.DMA
    out, fresh = pl.pallas_call(
        functools.partial(kernel, nz),
        out_shape=(
            jax.ShapeDtypeStruct((per, batch), bf16),
            jax.ShapeDtypeStruct((layers, 2, state, batch), f32),
        ),
        in_specs=[hbm] * 12,
        out_specs=(hbm, hbm),
        scratch_shapes=[
            pltpu.VMEM((per, batch), bf16),
            pltpu.VMEM((layers, per, ssm), bf16),
            pltpu.VMEM((2 * layers, per), bf16),
            pltpu.VMEM((layers, 1, state), f32),
            pltpu.VMEM((layers, 1, state), f32),
            pltpu.VMEM((1, layers), f32),
            pltpu.VMEM((layers, 2, ch, state), f32),
            pltpu.VMEM((layers, 2, ch, state), f32),
            pltpu.VMEM((layers, ch), f32),
            pltpu.VMEM((per, batch), bf16),
            pltpu.VMEM((width, batch), bf16),
            pltpu.VMEM((width, batch), bf16),
            pltpu.VMEM((layers, width, ssm), bf16),
            pltpu.VMEM((layers, ssm, batch), bf16),
            pltpu.VMEM((8, 128), f32),
            pltpu.VMEM((2 * nz * 8, 128), f32),
            pltpu.VMEM((width, 128), f32),
            pltpu.VMEM((width, 128), f32),
            pltpu.VMEM((layers, 2 * ch, width), bf16),
            pltpu.VMEM((layers, 128, 128), bf16),
            pltpu.VMEM((layers, 128, 128), f32),
            pltpu.VMEM((layers, ch, 2 * state), bf16),
            pltpu.VMEM((128, 128), f32),
            pltpu.VMEM((128, 128), f32),
            pltpu.VMEM((layers, 2, state, batch), f32),
            pltpu.VMEM((layers, 2, state, batch), f32),
            pltpu.VMEM((2 * ch, batch), f32),
            dma((2, half, 2, X_PIECES)),
            dma((half + 1,)),
            dma((layers, 2, half, 2, W_PIECES)),
            dma((layers, half + 1)),
            dma((layers, 2, half, 2, 1)),
            dma((layers, half + 1)),
            dma((2, half, 2, 1)),
            dma((half + 1,)),
            dma((14,)),
            dma((3,)),
            dma((12,)),
        ],
        compiler_params=pltpu.CompilerParams(
            collective_id=0, has_side_effects=True, vmem_limit_bytes=VMEM_MIB * 1024 * 1024
        ),
    )(
        tokens.T,
        carried.reshape(layers, 2, state, batch),
        proj_in.transpose(0, 2, 1),
        proj_gate.transpose(0, 2, 1),
        proj_out.transpose(0, 2, 1),
        norm.reshape(2 * layers, per),
        lam_re,
        lam_im,
        log_step.T,
        in_c.reshape(layers, 2, state, ch).transpose(0, 1, 3, 2),
        out_c.reshape(layers, 2, ch, state),
        skip,
    )
    out, fresh = pl.pallas_call(
        hand_out,
        out_shape=(
            jax.ShapeDtypeStruct((per, batch), bf16),
            jax.ShapeDtypeStruct((layers, 2, state, batch), f32),
        ),
        in_specs=[hbm, hbm],
        out_specs=(hbm, hbm),
        scratch_shapes=[
            pltpu.VMEM((per, batch), bf16),
            pltpu.VMEM((layers, 2, state, batch), f32),
            dma((2, 1 + 2 * layers)),
        ],
    )(out, fresh)
    return out.T, fresh.reshape(carried.shape)


def solution(mesh):
    return jax.shard_map(
        functools.partial(per_device, mesh.shape["tp"] // 2),
        mesh=mesh,
        in_specs=(
            P("grp", "tp"),
            P(None, None, "tp", None, "grp"),
            P(None, None, "tp"),
            P(None, None, "tp"),
            P(None, None, "tp"),
            P(None, None, "tp"),
            P(None, "tp", None),
            P(None, "tp", None),
            P(None, "tp"),
            P(None, None, "tp", None, None),
            P(None, None, "tp", None, None),
            P(None, "tp"),
        ),
        out_specs=(P("grp", "tp"), P(None, None, "tp", None, "grp")),
        check_vma=False,
    )
```

```python
import functools

import jax
import jax.numpy as jnp
from jax import lax
from jax.experimental import pallas as pl
from jax.experimental.pallas import tpu as pltpu
from jax.sharding import PartitionSpec as P

MESH = pl.DeviceIdType.MESH
bf16, f32 = jnp.bfloat16, jnp.float32

residual_scale = 1.4142135623730951
norm_eps = 1e-05

X_PIECES = 2
W_PIECES = 2
STRIDE = 2
EARLY = 1
SPAN = 1024
TALL = 2048
GAIN_ROWS = 512
W_LEAD = 6
VMEM_MIB = 56
W_RELAY = (1, 0)
P_RELAY = 1


def tile(start, size):
    return pl.ds(pl.multiple_of(start, size), size)


class Place:
    def __init__(self, nz):
        me = lax.axis_index("tp")
        self.nz, self.half = nz, nz // 2
        self.me, self.z, self.c = me, me // 2, lax.rem(me, 2)
        self.sib = self.z * 2 + (1 - self.c)

    def away(self, way, s):
        return lax.rem(self.z + (s if way == 0 else self.nz - s), self.nz)

    def origin(self, way, s):
        return self.away(1 - way, s)

    def carries(self, way, s, core):
        return s < self.half or (s == self.half and (way == 0) == (core == 1))


class Gather:
    def __init__(self, at, relay, own, buf, per, pieces, stride, send, recv, give, take):
        self.relay, self.relays = relay, at.c == relay
        self.at, self.own, self.buf, self.per, self.pieces, self.stride = at, own, buf, per, pieces, stride
        self.send_sem, self.recv_sem, self.give_sem, self.take_sem = send, recv, give, take

    def rows(self, start, size):
        return self.buf.at[pl.ds(pl.multiple_of(start, size), size)]

    def copy(self, way, s, core, i, by=1):
        at, size = self.at, self.per // self.pieces
        chip = at.origin(way, s - by)
        dst = self.rows((chip * 2 + core) * self.per + i * size, size)
        src = dst if s > by or self.own is None else self.own.at[pl.ds(i * size, size)]
        return pltpu.make_async_remote_copy(
            src_ref=src,
            dst_ref=dst,
            send_sem=self.send_sem,
            recv_sem=self.recv_sem.at[way, s - 1, core, i],
            device_id={"tp": at.away(way, by) * 2 + self.relay},
            device_id_type=MESH,
        )

    def arrive(self, way, s, core, i):
        size = self.per // self.pieces
        dst = self.rows((self.at.origin(way, s) * 2 + core) * self.per + i * size, size)
        pltpu.make_async_remote_copy(
            src_ref=dst,
            dst_ref=dst,
            send_sem=self.send_sem,
            recv_sem=self.recv_sem.at[way, s - 1, core, i],
            device_id={"tp": self.at.sib},
            device_id_type=MESH,
        ).wait_recv()

    def reach(self, s):
        if s % self.stride:
            return []
        return [s + by for by in range(self.stride, 0, -1) if s + by <= self.at.half]

    def span(self, way, s):
        chip = self.at.origin(way, s) * 2 * self.per
        if s < self.at.half:
            return self.rows(chip, 2 * self.per)
        return self.rows(chip + (self.per if way == 0 else 0), self.per)

    def handover(self, way, s):
        dst = self.span(way, s)
        return pltpu.make_async_remote_copy(
            src_ref=dst,
            dst_ref=dst,
            send_sem=self.give_sem,
            recv_sem=self.take_sem.at[s],
            device_id={"tp": self.at.sib},
            device_id_type=MESH,
        )

    def own_over(self):
        dst = self.rows(self.at.me * self.per, self.per)
        return pltpu.make_async_remote_copy(
            src_ref=dst if self.own is None else self.own,
            dst_ref=dst,
            send_sem=self.give_sem,
            recv_sem=self.take_sem.at[0],
            device_id={"tp": self.at.sib},
            device_id_type=MESH,
        )

    def sends(self, s, way, core):
        return [t for t in self.reach(s) if self.at.carries(way, t, core)]

    def begin(self):
        for core in range(2):

            @pl.when(self.at.c == core)
            def _():
                for t in self.reach(0):
                    for i in range(self.pieces):
                        for way in range(2):
                            if self.at.carries(way, t, core):
                                self.copy(way, t, core, i, t).start()

        self.own_over().start()

    def order(self):
        half, stride = self.at.half, self.stride
        out = []
        for k in range(0, half, stride):
            top = min(k + stride, half)
            out.append([top] + list(range(k + 1, top)))
        return out

    def step(self, s):
        @pl.when(self.relays)
        def _():
            for core in (self.relay, 1 - self.relay):
                for i in range(self.pieces):
                    for way in range(2):
                        if self.at.carries(way, s, core):
                            self.arrive(way, s, core, i)
                            for t in self.sends(s, way, core):
                                self.copy(way, t, core, i, t - s).start()
            for way in range(2):
                self.handover(way, s).start()

    def bulk(self, blocks, send=None, recv=None):
        ref = self.buf.at[pl.ds(0, blocks * self.per)]
        return pltpu.make_async_remote_copy(
            src_ref=ref,
            dst_ref=ref,
            send_sem=self.send_sem if send is None else send,
            recv_sem=self.take_sem.at[0] if recv is None else recv,
            device_id={"tp": self.at.sib},
            device_id_type=MESH,
        )

    def ready(self, s):
        if s == 0:
            self.bulk(1, recv=self.take_sem.at[0]).wait_recv()
            return

        @pl.when(jnp.logical_not(self.relays))
        def _():
            self.bulk(4 if s < self.at.half else 2, recv=self.take_sem.at[s]).wait_recv()

    def finish(self):
        half, every = self.at.half, [(way, core) for way in range(2) for core in range(2)]
        for core in range(2):
            sent = sum(self.at.carries(way, t, core) for t in self.reach(0) for way in range(2))
            given = 1
            if core == self.relay:
                sent += sum(len(self.sends(s, *who)) for s in range(1, half + 1) for who in every)
                given += 4 * (half - 1) + 2

            @pl.when(self.at.c == core)
            def _():
                self.bulk(sent).wait_send()
                self.bulk(given, send=self.give_sem).wait_send()


def dot(a, b):
    return jnp.dot(a, b, preferred_element_type=f32)


def kernel(
    nz,
    tok_in,
    carried,
    win,
    wgate,
    wout_in,
    norm_in,
    lam_re_in,
    lam_im_in,
    log_step_in,
    in_c_in,
    out_c_in,
    skip_in,
    out_to,
    new_carried,
    tok,
    wout,
    norm,
    lam_re,
    lam_im,
    log_step,
    in_c,
    out_c,
    skip,
    out,
    x_all,
    s_all,
    w_all,
    g_all,
    p_own,
    p_all,
    gain_b,
    bias_b,
    w_in,
    push_w,
    push_t,
    read_w,
    cols,
    cols_t,
    held,
    fresh,
    acc,
    x_sem,
    xd_sem,
    w_sem,
    wd_sem,
    g_sem,
    gd_sem,
    p_sem,
    pd_sem,
    in_sem,
    io_sem,
    sent,
):
    layers, half = 2, nz // 2
    ndev = 2 * nz
    width, batch = x_all.shape
    per = tok.shape[0]
    ch = win.shape[1]
    state = held.shape[2]
    place = Place(nz)
    me = place.me

    def gather(relay, own, buf, rows, pieces, stride, sem, over, out):
        return Gather(place, relay, own, buf, rows, pieces, stride, sent.at[2 * out], sem, sent.at[2 * out + 1], over)

    xr = gather(1, tok, x_all, per, X_PIECES, 1, x_sem, xd_sem, 0)
    pr = gather(P_RELAY, p_own, p_all, 8, 1, 1, p_sem, pd_sem, 1)
    wr = [gather(W_RELAY[i], wout.at[i], w_all.at[i], per, W_PIECES, 1, w_sem.at[i], wd_sem.at[i], 2 + i) for i in range(layers)]
    gr = [gather(1, None, g_all.at[i], ch, 1, STRIDE, g_sem.at[i], gd_sem.at[i], 4 + i) for i in range(layers)]

    barrier = pltpu.get_barrier_semaphore()
    reach = {core: max((r.stride for r in (xr, pr, *wr, *gr) if r.relay == core), default=0) for core in range(2)}

    def near(core):
        return [(way, s) for way in range(2) for s in range(1, min(reach[core], half) + 1) if way == 0 or 2 * s < nz]

    def here(dev):
        pl.semaphore_signal(barrier, inc=1, device_id={"tp": dev}, device_id_type=MESH)

    for core in range(2):

        @pl.when(place.c == core)
        def _():
            for way, s in near(core):
                for other in range(2):
                    here(place.away(way, s) * 2 + other)

    here(place.sib)
    sources = (tok_in, norm_in, wout_in, lam_re_in, lam_im_in, log_step_in, in_c_in, out_c_in, skip_in, carried)
    targets = (tok, norm, wout, lam_re, lam_im, log_step, in_c, out_c, skip, held)
    loads = [pltpu.make_async_copy(a, b, in_sem.at[i]) for i, (a, b) in enumerate(zip(sources, targets))]
    for k, w in enumerate((win, wgate)):
        for l in range(layers):
            part = w_in.at[l, pl.ds(k * ch, ch)]
            loads.append(pltpu.make_async_copy(w.at[l], part, in_sem.at[len(sources) + 2 * k + l]))
    for load in loads:
        load.start()
    loads[0].wait()
    loads[1].wait()
    p_own[...] = jnp.zeros_like(p_own)
    p_own[0:4, 0:per] = norm[...].astype(f32)
    pl.semaphore_wait(barrier, len(near(0)) + len(near(1)) + 1)

    xr.begin()
    pr.begin()
    for i, load in enumerate(loads):
        if i > 1 and i != len(sources) - 1:
            load.wait()

    x_all[tile(me * per, per)] = tok[...]
    p_all[tile(me * 8, 8)] = p_own[...]
    for l in range(layers):
        w_all[l, tile(me * per, per)] = wout[l]
    cols[...] = jnp.zeros_like(cols)
    for l in range(layers):
        re, im = lam_re[l], lam_im[l]
        step_len = jnp.exp(log_step[0:1, l : l + 1])
        modulus = jnp.exp(re * step_len)
        decay_re = modulus * jnp.cos(im * step_len)
        decay_im = modulus * jnp.sin(im * step_len)
        denominator = re * re + im * im
        shifted = decay_re - 1.0
        coef_re = (shifted * re + decay_im * im) / denominator
        coef_im = (decay_im * re - shifted * im) / denominator
        in_re = coef_re * in_c[l, 0] - coef_im * in_c[l, 1]
        in_im = coef_re * in_c[l, 1] + coef_im * in_c[l, 0]
        push_t[l] = jnp.zeros_like(push_t[l])
        for k, v in enumerate((in_re, in_im)):
            high = v.astype(bf16).astype(f32)
            push_t[l, 0:ch, k * state : (k + 1) * state] = high
            push_t[l, ch : 2 * ch, k * state : (k + 1) * state] = v - high
        push_w[l] = push_t[l].T.astype(bf16)
        read_w[l, :, 0:state] = out_c[l, 0].astype(bf16)
        read_w[l, :, state : 2 * state] = (-out_c[l, 1]).astype(bf16)
        cols[8 * l : 8 * l + 1, 0:state] = decay_re
        cols[8 * l + 1 : 8 * l + 2, 0:state] = decay_im
        cols[8 * l + 2 : 8 * l + 3, 0:ch] = skip[l : l + 1]
    cols[3:5, 0:per] = norm[2:4].astype(f32)
    cols_t[...] = cols[...].T

    def gain_columns():
        for d in range(ndev):
            if d % 16 == 0:
                turned = p_all[d * 8 : d * 8 + min(128, ndev * 8)].T
            at = (d % 16) * 8
            gain_b[d * per : (d + 1) * per] = jnp.broadcast_to(turned[0:per, at : at + 1], (per, 128))
            bias_b[d * per : (d + 1) * per] = jnp.broadcast_to(turned[0:per, at + 1 : at + 2], (per, 128))

    def meet(dev_z):
        k = tile(dev_z * 2 * per, 2 * per)
        acc[...] += dot(w_in[0, :, k], x_all[k])

    acc[...] = jnp.zeros_like(acc)
    w_first = max(half + 1 - W_LEAD, 0)
    if w_first == 0:
        wr[0].begin()
    for s in range(1, half + 1):
        xr.step(s)
        if s == w_first:
            wr[0].begin()
        if s > w_first:
            wr[0].step(s - w_first)
        pr.step(s)
        xr.ready(s - 1)
        if s == 1:
            meet(place.z)
        else:
            for way in range(2):
                meet(place.origin(way, s - 1))
    if W_LEAD == 0:
        wr[0].begin()
    xr.ready(half)
    meet(place.origin(0, half))
    w_next = max(min(W_LEAD, half), 1) if w_first else half + 1

    loads[len(sources) - 1].wait()

    span = min(SPAN, batch)

    def recur(l, at):
        drive = acc[0:ch, at].astype(bf16)
        gate = acc[ch : 2 * ch, at].astype(bf16).astype(f32)
        pushed = dot(push_w[l, :, 0 : 2 * ch], jnp.concatenate([drive, drive], axis=0))
        decay_re = cols_t[0:state, 8 * l : 8 * l + 1]
        decay_im = cols_t[0:state, 8 * l + 1 : 8 * l + 2]
        old_re, old_im = held[l, 0, :, at], held[l, 1, :, at]
        re = decay_re * old_re - decay_im * old_im + pushed[0:state]
        im = decay_re * old_im + decay_im * old_re + pushed[state:]
        fresh[l, 0, :, at] = re
        fresh[l, 1, :, at] = im
        both = jnp.concatenate([re.astype(bf16), im.astype(bf16)], axis=0)
        y = dot(read_w[l], both) + cols_t[0:ch, 8 * l + 2 : 8 * l + 3] * drive.astype(f32)
        gated = jax.nn.gelu(y) * jax.nn.sigmoid(gate)
        g_all[l, tile(me * ch, ch), at] = gated.astype(bf16)

    def spans(work):
        def body(j, _):
            work(tile(j * span, span))
            return 0

        lax.fori_loop(0, batch // span, body, 0)

    def store(l):
        return pltpu.make_async_copy(fresh.at[l], new_carried.at[l], io_sem.at[l])

    w_two = iter(range(half + 1))

    def further():
        s = next(w_two, None)
        if s == 0:
            wr[1].begin()
        elif s is not None:
            wr[1].step(s)

    def exchange(l, left):
        gr[l].begin()
        order = gr[l].order()
        if l == 0:
            further()
            for s in range(half + 1):
                pr.ready(s)
            gain_columns()
        for n, steps in enumerate(order):
            for s in steps:
                gr[l].step(s)
            upto = -(-len(left) // (len(order) - n))
            for s in left[:upto]:
                wr[l].step(s)
            left = left[upto:]
            if l == 0:
                further()
        for s in range(half + 1):
            gr[l].ready(s)
            wr[l].ready(s)

    tall = min(TALL, width)

    def moments(l, src, keep, at):
        def body(t, sums):
            k = tile(t * tall, tall)
            mixed = dot(w_all[l, k], g_all[l, :, at])
            summed = (residual_scale * src[k, at].astype(f32) + mixed).astype(bf16)
            if keep is not None:
                keep[k, at] = summed
            wide = summed.astype(f32).reshape(tall // 8, 8, span)
            return sums[0] + wide.sum(axis=0), sums[1] + (wide * wide).sum(axis=0)

        zero = jnp.zeros((8, span), f32)
        total, squares = lax.fori_loop(0, width // tall, body, (zero, zero))
        mean = total.sum(axis=0, keepdims=True) / width
        var = squares.sum(axis=0, keepdims=True) / width - mean * mean
        return mean, lax.rsqrt(var + norm_eps)

    def first_norm(at):
        mean, scale = moments(0, x_all, s_all, at)
        gain_rows = min(GAIN_ROWS, width)

        def normed(t, _):
            k = tile(t * gain_rows, gain_rows)
            wide = (s_all[k, at].astype(f32) - mean) * scale
            gain, bias = gain_b[k], bias_b[k]
            pieces = [wide[:, i : i + 128] * gain + bias for i in range(0, span, 128)]
            s_all[k, at] = jnp.concatenate(pieces, axis=1).astype(bf16)
            return 0

        lax.fori_loop(0, width // gain_rows, normed, 0)
        acc[:, at] = dot(w_in[1], s_all[:, at])
        recur(1, at)

    mine = tile(me * per, per)

    def last_norm(at):
        mean, scale = moments(1, s_all, None, at)
        mixed = dot(wout[1], g_all[1, :, at])
        summed = (residual_scale * s_all[mine, at].astype(f32) + mixed).astype(bf16).astype(f32)
        out[:, at] = ((summed - mean) * scale * cols_t[0:per, 3:4] + cols_t[0:per, 4:5]).astype(bf16)

    spans(functools.partial(recur, 0))
    store(0).start()
    exchange(0, list(range(w_next, half + 1)))
    spans(first_norm)
    store(1).start()
    if EARLY:
        further()
    exchange(1, list(w_two))
    spans(last_norm)
    last = pltpu.make_async_copy(out, out_to, io_sem.at[2])
    last.start()
    store(0).wait()
    store(1).wait()
    last.wait()
    for ring in (xr, pr, *wr, *gr):
        ring.finish()


def hand_out(out_in, fresh_in, out, fresh, out_held, fresh_held, sem):
    layers = fresh.shape[0]
    pairs = [(out_in, out_held, out)]
    pairs += [(fresh_in.at[l, k], fresh_held.at[l, k], fresh.at[l, k]) for l in range(layers) for k in range(2)]
    into = [pltpu.make_async_copy(a, b, sem.at[0, i]) for i, (a, b, _) in enumerate(pairs)]
    onto = [pltpu.make_async_copy(b, c, sem.at[1, i]) for i, (_, b, c) in enumerate(pairs)]
    for copy in into:
        copy.start()
    for first, then in zip(into, onto):
        first.wait()
        then.start()
    for copy in onto:
        copy.wait()


def per_device(nz, tokens, carried, proj_in, proj_gate, proj_out, norm, lam_re, lam_im, log_step, in_c, out_c, skip):
    batch, per = tokens.shape
    layers, width, ch = proj_in.shape
    ssm = proj_out.shape[1]
    state = carried.shape[3]
    half = nz // 2
    hbm = pl.BlockSpec(memory_space=pl.ANY)
    dma = pltpu.SemaphoreType.DMA
    out, fresh = pl.pallas_call(
        functools.partial(kernel, nz),
        out_shape=(
            jax.ShapeDtypeStruct((per, batch), bf16),
            jax.ShapeDtypeStruct((layers, 2, state, batch), f32),
        ),
        in_specs=[hbm] * 12,
        out_specs=(hbm, hbm),
        scratch_shapes=[
            pltpu.VMEM((per, batch), bf16),
            pltpu.VMEM((layers, per, ssm), bf16),
            pltpu.VMEM((2 * layers, per), bf16),
            pltpu.VMEM((layers, 1, state), f32),
            pltpu.VMEM((layers, 1, state), f32),
            pltpu.VMEM((1, layers), f32),
            pltpu.VMEM((layers, 2, ch, state), f32),
            pltpu.VMEM((layers, 2, ch, state), f32),
            pltpu.VMEM((layers, ch), f32),
            pltpu.VMEM((per, batch), bf16),
            pltpu.VMEM((width, batch), bf16),
            pltpu.VMEM((width, batch), bf16),
            pltpu.VMEM((layers, width, ssm), bf16),
            pltpu.VMEM((layers, ssm, batch), bf16),
            pltpu.VMEM((8, 128), f32),
            pltpu.VMEM((2 * nz * 8, 128), f32),
            pltpu.VMEM((width, 128), f32),
            pltpu.VMEM((width, 128), f32),
            pltpu.VMEM((layers, 2 * ch, width), bf16),
            pltpu.VMEM((layers, 128, 128), bf16),
            pltpu.VMEM((layers, 128, 128), f32),
            pltpu.VMEM((layers, ch, 2 * state), bf16),
            pltpu.VMEM((128, 128), f32),
            pltpu.VMEM((128, 128), f32),
            pltpu.VMEM((layers, 2, state, batch), f32),
            pltpu.VMEM((layers, 2, state, batch), f32),
            pltpu.VMEM((2 * ch, batch), f32),
            dma((2, half, 2, X_PIECES)),
            dma((half + 1,)),
            dma((layers, 2, half, 2, W_PIECES)),
            dma((layers, half + 1)),
            dma((layers, 2, half, 2, 1)),
            dma((layers, half + 1)),
            dma((2, half, 2, 1)),
            dma((half + 1,)),
            dma((14,)),
            dma((3,)),
            dma((12,)),
        ],
        compiler_params=pltpu.CompilerParams(
            collective_id=0, has_side_effects=True, vmem_limit_bytes=VMEM_MIB * 1024 * 1024
        ),
    )(
        tokens.T,
        carried.reshape(layers, 2, state, batch),
        proj_in.transpose(0, 2, 1),
        proj_gate.transpose(0, 2, 1),
        proj_out.transpose(0, 2, 1),
        norm.reshape(2 * layers, per),
        lam_re,
        lam_im,
        log_step.T,
        in_c.reshape(layers, 2, state, ch).transpose(0, 1, 3, 2),
        out_c.reshape(layers, 2, ch, state),
        skip,
    )
    out, fresh = pl.pallas_call(
        hand_out,
        out_shape=(
            jax.ShapeDtypeStruct((per, batch), bf16),
            jax.ShapeDtypeStruct((layers, 2, state, batch), f32),
        ),
        in_specs=[hbm, hbm],
        out_specs=(hbm, hbm),
        scratch_shapes=[
            pltpu.VMEM((per, batch), bf16),
            pltpu.VMEM((layers, 2, state, batch), f32),
            dma((2, 1 + 2 * layers)),
        ],
    )(out, fresh)
    return out.T, fresh.reshape(carried.shape)


def solution(mesh):
    return jax.shard_map(
        functools.partial(per_device, mesh.shape["tp"] // 2),
        mesh=mesh,
        in_specs=(
            P("grp", "tp"),
            P(None, None, "tp", None, "grp"),
            P(None, None, "tp"),
            P(None, None, "tp"),
            P(None, None, "tp"),
            P(None, None, "tp"),
            P(None, "tp", None),
            P(None, "tp", None),
            P(None, "tp"),
            P(None, None, "tp", None, None),
            P(None, None, "tp", None, None),
            P(None, "tp"),
        ),
        out_specs=(P("grp", "tp"), P(None, None, "tp", None, "grp")),
        check_vma=False,
    )
```
